32 devices in a mesh: sp: 8 (over z, y), tp: 4 (over x, core).
Axes of the slice: x: 2, y: 2, z: 4, core: 2. Of those that a mesh axis runs over, the one named last changes fastest.
Arguments:
- tokens: bfloat16 [4096, 2048], P('sp', 'tp'), may hold values from -64 to 64
- conv_input: bfloat16 [2048, 1024], P(None, 'tp'), may hold values from -0.125 to 0.125
- conv_inner: bfloat16 [2048, 1024], P(None, 'tp'), may hold values from -0.125 to 0.125
- conv_outer: bfloat16 [2048, 1024], P(None, 'tp'), may hold values from -0.125 to 0.125
- conv_gate: bfloat16 [2048, 1024], P(None, 'tp'), may hold values from -0.125 to 0.125
- conv_taps: bfloat16 [3, 1024], P(None, 'tp'), may hold values from -3.5 to 3.5
- query_proj: bfloat16 [2048, 1536], P(None, 'tp'), may hold values from -8 to 8
- latent_proj: bfloat16 [2048, 256], replicated, may hold values from -1 to 1
- rope_proj: bfloat16 [2048, 32], replicated, may hold values from -0.125 to 0.125
- latent_gain: float32 [256], replicated, may hold values from 0.1 to 1.9
- key_up: bfloat16 [256, 1024], P(None, 'tp'), may hold values from -2 to 2
- value_up: bfloat16 [256, 1024], P(None, 'tp'), may hold values from -0.375 to 0.375
- attn_gate: bfloat16 [2048, 1024], P(None, 'tp'), may hold values from -0.125 to 0.125
- conv_down: bfloat16 [1024, 2048], P('tp'), may hold values from -0.1875 to 0.1875
- attn_down: bfloat16 [1024, 2048], P('tp'), may hold values from -0.75 to 0.75
Outputs:
- layer_out: bfloat16 [4096, 2048], P(('sp', 'tp'))
The draws below stay inside these ranges and needn't reach their ends.
All inputs are finite; a program needn't handle non-finite values.
Results may differ from the reference program's by a relative error of at most 0.014.
Values may be sent and summed in bfloat16 or wider, within the bound.
A program may use at most 128 MiB of HBM per device.

```python
import math
import jax
import jax.numpy as jnp
from jax import lax

D = 2048
D_CONV = 1024
HEADS = 16
NOPE = 64
ROPE = 32
VDIM = 64
KV = 256
GRID_W = 64
SEQ = 4096
N_TP = 4


def weight_pair(key):
    down_part = jnp.clip(jax.random.normal(jax.random.fold_in(key, 101), (D, KV), jnp.float32), -6.0, 6.0) * D ** (-0.5)
    up_part = jnp.clip(jax.random.normal(jax.random.fold_in(key, 102), (KV, HEADS * NOPE), jnp.float32), -6.0, 6.0) * KV ** (-0.5)
    return (down_part, up_part)


def draw_latent_proj(key, part):
    return jnp.clip(weight_pair(key)[0], -1.0, 1.0).astype(jnp.bfloat16)


def draw_key_up(key, part):
    return jnp.clip(weight_pair(key)[1], -2.0, 2.0).astype(jnp.bfloat16)


def draw_tokens(key, part):
    column = jnp.arange(D, dtype=jnp.float32) / max(D - 1, 1)
    col_noise = jax.random.uniform(jax.random.fold_in(key, 201), (D,), jnp.float32)
    row_exp = jax.random.uniform(jax.random.fold_in(key, 202), (SEQ,), jnp.float32, -0.5, 0.5)
    base_draw = jnp.clip(jax.random.normal(jax.random.fold_in(key, 204), (SEQ, D), jnp.float32), -6.0, 6.0)
    col_exp = 0.5 * column + 0.5 * col_noise - 0.5
    scaling = (10.0 ** row_exp)[:, None] * (10.0 ** col_exp)[None, :]
    values = base_draw * scaling
    return jnp.clip(values, -64.0, 64.0).astype(jnp.bfloat16)


def draw_query_proj(key, part):
    spread = (6.0 / D) ** 0.5
    whole_draw = jnp.clip(jax.random.normal(jax.random.fold_in(key, 303), (D, HEADS, NOPE + ROPE), jnp.float32), -6.0, 6.0) * spread
    return jnp.clip(whole_draw, -8.0, 8.0).reshape(D, HEADS * (NOPE + ROPE)).astype(jnp.bfloat16)


def block_levels(rng, shape, cuts, low, high):
    gain = 1.0
    for axis_at, shards_of in cuts:
        draws = jax.random.uniform(jax.random.fold_in(jax.random.fold_in(rng, 6), axis_at), (shards_of,), jnp.float32, low / len(cuts), high / len(cuts))
        gain = gain * jnp.repeat(jnp.exp(draws), shape[axis_at] // shards_of).reshape((-1,) + (1,) * (len(shape) - 1 - axis_at))
    return gain


def bell_draw(key, shape, width, bound, split=(), kind=jnp.bfloat16):
    array = width * jax.random.normal(key, shape, jnp.float32)
    if split:
        array = array * block_levels(key, shape, split, -0.22, 0.18)
    return jnp.clip(array, -bound, bound).astype(kind)


def setup_inputs(seed: int = 0) -> dict:
    splits = jax.random.split(jax.random.key(seed), 16)
    return {
        "tokens": draw_tokens(jax.random.fold_in(splits[15], 71), 0),
        "conv_input": bell_draw(splits[1], (D, D_CONV), D ** -0.5, 0.125, ((1, 4),)),
        "conv_inner": bell_draw(splits[2], (D, D_CONV), D ** -0.5, 0.125, ((1, 4),)),
        "conv_outer": bell_draw(splits[3], (D, D_CONV), D ** -0.5, 0.125, ((1, 4),)),
        "conv_gate": bell_draw(splits[4], (D, D_CONV), D ** -0.5, 0.125, ((1, 4),)),
        "conv_taps": bell_draw(splits[5], (3, D_CONV), 3 ** -0.5, 3.5, ((1, 4),)),
        "query_proj": draw_query_proj(jax.random.fold_in(splits[15], 71), 0),
        "latent_proj": draw_latent_proj(jax.random.fold_in(splits[15], 71), 0),
        "rope_proj": bell_draw(splits[8], (D, ROPE), D ** -0.5, 0.125),
        "latent_gain": jnp.clip(1.0 + 0.18 * jax.random.normal(splits[9], (KV,), jnp.float32), 0.1, 1.9),
        "key_up": draw_key_up(jax.random.fold_in(splits[15], 71), 0),
        "value_up": bell_draw(splits[11], (KV, HEADS * VDIM), KV ** -0.5, 0.375, ((1, 4),)),
        "attn_gate": bell_draw(splits[12], (D, HEADS * VDIM), D ** -0.5, 0.125, ((1, 4),)),
        "conv_down": bell_draw(splits[13], (D_CONV, D), D_CONV ** -0.5, 0.1875, ((0, 4),)),
        "attn_down": bell_draw(splits[14], (HEADS * VDIM, D), (HEADS * VDIM // 16) ** -0.5, 0.75, ((0, 4),)),
    }


rms_eps = 1e-06
rope_theta = 10000.0

def rounded(values):
    return lax.optimization_barrier(values.astype(jnp.bfloat16))

def axial_tables(positions, rope_width, grid_width):
    quarter = rope_width // 4
    frequency = rope_theta ** (-jnp.arange(quarter, dtype=jnp.float32) * 2.0 / (rope_width // 2))
    grid_row = (positions // grid_width).astype(jnp.float32)
    grid_col = (positions % grid_width).astype(jnp.float32)
    row_angle = grid_row[:, None] * frequency[None, :]
    col_angle = grid_col[:, None] * frequency[None, :]
    return (jnp.cos(row_angle), jnp.sin(row_angle), jnp.cos(col_angle), jnp.sin(col_angle))

def turn_half(vector, cos_table, sin_table):
    half_width = vector.shape[-1] // 2
    leading = vector[..., :half_width]
    trailing = vector[..., half_width:]
    return jnp.concatenate([leading * cos_table - trailing * sin_table, trailing * cos_table + leading * sin_table], axis=-1)

def axial_turn(vector, tables):
    half_width = vector.shape[-1] // 2
    return jnp.concatenate([turn_half(vector[..., :half_width], tables[0], tables[1]), turn_half(vector[..., half_width:], tables[2], tables[3])], axis=-1)

def reference(tokens, conv_input, conv_inner, conv_outer, conv_gate, conv_taps, query_proj, latent_proj, rope_proj, latent_gain, key_up, value_up, attn_gate, conv_down, attn_down):
    seq_len = tokens.shape[0]
    widened = tokens.astype(jnp.float32)
    row_scale = lax.rsqrt(lax.optimization_barrier(jnp.mean(widened * widened, axis=1, keepdims=True)) + rms_eps)

    def project(matrix):
        return jnp.dot(tokens, matrix, preferred_element_type=jnp.float32) * row_scale
    value_in = rounded(project(conv_input)).astype(jnp.float32)
    inner_in = rounded(project(conv_inner)).astype(jnp.float32)
    outer_in = rounded(project(conv_outer)).astype(jnp.float32)
    gate_in = rounded(project(conv_gate)).astype(jnp.float32)
    conv_product = rounded(inner_in * value_in).astype(jnp.float32)
    padded = jnp.pad(conv_product, ((1, 1), (0, 0)))
    tap_weights = conv_taps.astype(jnp.float32)
    conv_mixed = padded[:-2] * tap_weights[0] + padded[1:-1] * tap_weights[1] + padded[2:] * tap_weights[2]
    conv_out = (jax.nn.silu(gate_in) * outer_in * conv_mixed).astype(jnp.bfloat16)
    positions = jnp.arange(seq_len, dtype=jnp.int32)
    tables = axial_tables(positions, ROPE, GRID_W)
    head_tables = tuple((grid_table[:, None, :] for grid_table in tables))
    queries = project(query_proj).reshape(seq_len, HEADS, NOPE + ROPE)
    query_nope = queries[..., :NOPE].astype(jnp.bfloat16)
    query_rope = axial_turn(queries[..., NOPE:], head_tables).astype(jnp.bfloat16)
    latent = project(latent_proj)
    latent = (latent * lax.rsqrt(lax.optimization_barrier(jnp.mean(latent * latent, axis=1, keepdims=True)) + rms_eps) * latent_gain).astype(jnp.bfloat16)
    key_rope = axial_turn(project(rope_proj), tables).astype(jnp.bfloat16)
    key_nope = jnp.dot(latent, key_up, preferred_element_type=jnp.float32).astype(jnp.bfloat16).reshape(seq_len, HEADS, NOPE)
    key_values = jnp.dot(latent, value_up, preferred_element_type=jnp.float32).astype(jnp.bfloat16).reshape(seq_len, HEADS, VDIM)
    gate_attn = rounded(project(attn_gate)).astype(jnp.float32)
    key_wide = key_nope.astype(jnp.float32)
    rope_wide = key_rope.astype(jnp.float32)
    value_wide = key_values.astype(jnp.float32)
    block_rows = math.gcd(seq_len, 256)
    score_scale = (NOPE + ROPE) ** (-0.5)

    def attend_block(block_pair):
        nope_block, rope_block = block_pair
        scores = jnp.einsum('qhd,khd->hqk', nope_block.astype(jnp.float32), key_wide)
        scores = (scores + jnp.einsum('qhd,kd->hqk', rope_block.astype(jnp.float32), rope_wide)) * score_scale
        row_top = lax.optimization_barrier(jnp.max(scores, axis=2, keepdims=True))
        weights = jnp.exp(scores - row_top)
        weight_total = lax.optimization_barrier(jnp.sum(weights, axis=2))
        narrow = rounded(weights).astype(jnp.float32)
        attended = jnp.einsum('hqk,khd->qhd', narrow, value_wide) / weight_total.T[:, :, None]
        return attended.reshape(attended.shape[0], HEADS * VDIM)
    attended = lax.map(attend_block, (query_nope.reshape(-1, block_rows, HEADS, NOPE), query_rope.reshape(-1, block_rows, HEADS, ROPE)))
    attended = attended.reshape(seq_len, HEADS * VDIM)
    attn_out = (jax.nn.silu(gate_attn) * attended).astype(jnp.bfloat16)
    conv_width = D_CONV // N_TP
    head_width = HEADS // N_TP * VDIM
    conv_groups = conv_out.reshape(seq_len, N_TP, conv_width).transpose(1, 0, 2)
    attn_groups = attn_out.reshape(seq_len, N_TP, head_width).transpose(1, 0, 2)
    conv_blocks = conv_down.reshape(N_TP, conv_width, conv_down.shape[1])
    attn_blocks = attn_down.reshape(N_TP, head_width, attn_down.shape[1])

    def add_group(running_sum, group_terms):
        conv_part, conv_matrix, attn_part, attn_matrix = group_terms
        partial_sum = jnp.dot(conv_part, conv_matrix, preferred_element_type=jnp.float32) + jnp.dot(attn_part, attn_matrix, preferred_element_type=jnp.float32)
        return (running_sum + rounded(partial_sum).astype(jnp.float32), None)
    zeroed = jnp.zeros((seq_len, conv_down.shape[1]), jnp.float32)
    summed = lax.scan(add_group, zeroed, (conv_groups, conv_blocks, attn_groups, attn_blocks))[0]
    return summed.astype(jnp.bfloat16)
```

```python
import functools
import math

import jax
import jax.numpy as jnp
from jax import lax
from jax.experimental import pallas as pl
from jax.experimental.pallas import tpu as pltpu
from jax.sharding import PartitionSpec as P

NOPE = 64
ROPE = 32
VDIM = 64
GRID_W = 64
LANES = 128
rms_eps = 1e-06
rope_theta = 10000.0
MESH = pl.DeviceIdType.MESH
BF = jnp.bfloat16
F32 = jnp.float32


def silu(v):
    return v / (1.0 + jnp.exp(-v))


def dot(a, b):
    return jnp.dot(a, b, preferred_element_type=F32)


def body(
    dims,
    tokens, wci, wcn, wco, wcg, wq, wg, wl, wr, cd, ad, taps, gain, ku, vu,
    out,
    x_all, w_conv, w_q, w_g, w_lr, w_down, kv, kbuf, vbuf, qbuf, scl, cosb, sina, sinb,
    cprod, cgo, gat, halo, mix, mbuf, acc, sbuf, pbuf, xbuf, rbuf, ybuf,
    wsem, tsend, trecv, rsend, rrecv, ksend, krecv, psend, precv, hsend, hrecv,
    dsend, drecv, xsend, xrecv,
):
    n_sp, n_tp, R, fl, D, H, C, KV, NC = dims
    X = n_tp // 2
    RG = R // X
    TB = R // n_tp
    RC = R // NC
    HB = R // 2
    HR = HB // 8
    sp = lax.axis_index("sp")
    tp = lax.axis_index("tp")
    chip = tp // 2
    core = tp % 2
    mate = chip * 2 + (1 - core)

    loads = [
        pltpu.make_async_copy(wl, w_lr.at[:, 0:KV], wsem.at[0]),
        pltpu.make_async_copy(wr, w_lr.at[:, KV:KV + LANES], wsem.at[1]),
        pltpu.make_async_copy(wcn, w_conv.at[0], wsem.at[2]),
        pltpu.make_async_copy(wci, w_conv.at[1], wsem.at[3]),
        pltpu.make_async_copy(wco, w_conv.at[2], wsem.at[4]),
        pltpu.make_async_copy(wcg, w_conv.at[3], wsem.at[5]),
        pltpu.make_async_copy(wq, w_q, wsem.at[6]),
        pltpu.make_async_copy(wg, w_g, wsem.at[7]),
        pltpu.make_async_copy(cd, w_down.at[0:C, :], wsem.at[8]),
        pltpu.make_async_copy(ad, w_down.at[C:, :], wsem.at[9]),
    ]

    def cols(j):
        return pl.ds(pl.multiple_of(j * fl, fl), fl)

    own = pltpu.make_async_copy(tokens, x_all.at[:, cols(tp)], wsem.at[10])

    barrier = pltpu.get_barrier_semaphore()
    pl.semaphore_signal(barrier, inc=1, device_id={"tp": mate}, device_id_type=MESH)
    for d in range(1, X):
        peer = ((chip + d) % X) * 2 + core
        pl.semaphore_signal(barrier, inc=1, device_id={"tp": peer}, device_id_type=MESH)
    for d in range(1, n_sp):
        pl.semaphore_signal(barrier, inc=1, device_id={"sp": (sp + d) % n_sp}, device_id_type=MESH)
    own.start()
    pl.semaphore_wait(barrier, 1 + (X - 1) + (n_sp - 1))

    def send_tok(d, c):
        peer = mate if d == 0 else ((chip + d) % X) * 2 + core
        rows = pl.ds(c * RC, RC)
        return pltpu.make_async_remote_copy(
            src_ref=tokens.at[rows], dst_ref=x_all.at[rows, cols(tp)],
            send_sem=tsend.at[d, c], recv_sem=trecv.at[d, c],
            device_id={"tp": peer}, device_id_type=MESH)

    def relay_tok(d, c):
        origin = ((chip - d + X) % X) * 2 + core
        rows = pl.ds(c * RC, RC)
        part = x_all.at[rows, cols(origin)]
        return pltpu.make_async_remote_copy(
            src_ref=part, dst_ref=part,
            send_sem=rsend.at[d, c], recv_sem=rrecv.at[d, c],
            device_id={"tp": mate}, device_id_type=MESH)

    for c in range(NC):
        for d in range(1, X):
            send_tok(d, c).start()
    for c in range(NC):
        send_tok(0, c).start()
    for w in loads:
        w.start()

    lane = lax.broadcasted_iota(jnp.int32, (R, LANES), 1)
    pos = sp * R + lax.broadcasted_iota(jnp.int32, (R, LANES), 0)
    rl = lane - NOPE
    grid = jnp.where(rl < ROPE // 2, pos // GRID_W, pos % GRID_W).astype(F32)
    freq = jnp.exp((lane % 8).astype(F32) * (-math.log(rope_theta) / 8.0))
    ang = grid * freq
    active = (lane >= NOPE) & (lane < NOPE + ROPE)
    first = (lane % 16) < 8
    sin = jnp.sin(ang)
    cosb[...] = jnp.where(active, jnp.cos(ang), 0.0)
    sina[...] = jnp.where(active & first, -sin, 0.0)
    sinb[...] = jnp.where(active & (~first), sin, 0.0)

    def turned(v, rows):
        return (pltpu.roll(v, LANES - 8, 1) * sina[rows, :]
                + pltpu.roll(v, 8, 1) * sinb[rows, :])

    own.wait()
    loads[0].wait()
    loads[1].wait()
    for c in range(NC):
        for d in range(1, X):
            send_tok(d, c).wait_recv()
            relay_tok(d, c).start()
        send_tok(0, c).wait_recv()
        for d in range(1, X):
            relay_tok(d, c).wait_recv()
        rows = pl.ds(c * RC, RC)
        xr = x_all[rows, :]
        xf = xr.astype(F32)
        sc = lax.rsqrt(jnp.sum(xf * xf, axis=1, keepdims=True) * (1.0 / D) + rms_eps)
        scl[rows, :] = jnp.broadcast_to(sc, (RC, LANES))
        z = dot(xr, w_lr[...]) * sc
        lat = z[:, :KV]
        lat = lat * lax.rsqrt(jnp.mean(lat * lat, axis=1, keepdims=True) + rms_eps) * gain[...]
        half, off = (c * RC) // HB, (c * RC) % HB
        kv[sp, half, off:off + RC, :] = lat.astype(BF)
        rp = z[:, KV:]
        mix[rows, 0:LANES] = rp * cosb[rows, :] + turned(rp, rows)
    for half in range(2):
        packed = []
        for g in range(2):
            total = jnp.zeros((HR, LANES), F32)
            for b in range(4):
                r0 = half * HB + (g * 4 + b) * HR
                total = total + pltpu.roll(mix[r0:r0 + HR, 0:LANES], (32 * b - NOPE) % LANES, 1)
            packed.append(total)
        kv[sp, half, HB:HB + HR, :] = jnp.concatenate(packed, axis=1).astype(BF)

    def send_kv(d):
        part = kv.at[sp, core]
        return pltpu.make_async_remote_copy(
            src_ref=part, dst_ref=part, send_sem=ksend.at[d], recv_sem=krecv.at[sp],
            device_id={"sp": (sp + d) % n_sp}, device_id_type=MESH)

    def recv_kv(o):
        part = kv.at[o, core]
        return pltpu.make_async_remote_copy(
            src_ref=part, dst_ref=part, send_sem=ksend.at[0], recv_sem=krecv.at[o],
            device_id={"tp": mate}, device_id_type=MESH)

    def relay_kv(o, which):
        part = kv.at[o, which]
        return pltpu.make_async_remote_copy(
            src_ref=part, dst_ref=part, send_sem=psend.at[o], recv_sem=precv.at[o],
            device_id={"tp": mate}, device_id_type=MESH)

    order = []
    for i in range(1, n_sp):
        order.append((i + 1) // 2 if i % 2 else n_sp - i // 2)
    for d in order:
        send_kv(d).start()

    for w in loads[2:6]:
        w.wait()
    PB = min(R, 256)

    @pl.loop(0, R // PB)
    def _(i):
        rows = pl.ds(pl.multiple_of(i * PB, PB), PB)
        xr = x_all[rows, :]
        sc = scl[rows, 0:1]
        inner = (dot(xr, w_conv[0]) * sc).astype(BF).astype(F32)
        value = (dot(xr, w_conv[1]) * sc).astype(BF).astype(F32)
        cprod[rows, :] = (inner * value).astype(BF)
        outer = (dot(xr, w_conv[2]) * sc).astype(BF).astype(F32)
        gate = (dot(xr, w_conv[3]) * sc).astype(BF).astype(F32)
        cgo[rows, :] = silu(gate) * outer

    EDGE = 16

    def send_halo(k):
        src = cprod.at[pl.ds(R - EDGE, EDGE)] if k == 0 else cprod.at[pl.ds(0, EDGE)]
        to = (sp + 1) % n_sp if k == 0 else (sp + n_sp - 1) % n_sp
        return pltpu.make_async_remote_copy(
            src_ref=src, dst_ref=halo.at[k], send_sem=hsend.at[k], recv_sem=hrecv.at[k],
            device_id={"sp": to}, device_id_type=MESH)

    send_halo(0).start()
    send_halo(1).start()
    loads[6].wait()
    loads[7].wait()

    @pl.loop(0, R // PB)
    def _(i):
        rows = pl.ds(pl.multiple_of(i * PB, PB), PB)
        xr = x_all[rows, :]
        sc = scl[rows, 0:1]
        q = dot(xr, w_q[...]) * sc
        ln = lax.broadcasted_iota(jnp.int32, (PB, LANES), 1)
        for h in range(H):
            v = q[:, h * LANES:(h + 1) * LANES]
            v = v * jnp.where(ln < NOPE, 1.0, cosb[rows, :]) + turned(v, rows)
            qbuf[h, rows, :] = v.astype(BF)
        gat[rows, :] = silu((dot(xr, w_g[...]) * sc).astype(BF).astype(F32))

    def build(o):
        ln = lax.broadcasted_iota(jnp.int32, (HR, LANES), 1)
        keep = (ln >= NOPE) & (ln < NOPE + ROPE)
        ones = jnp.where(lax.broadcasted_iota(jnp.int32, (HB, LANES), 1) == VDIM, 1.0, 0.0)
        for half in range(2):
            lat = kv[o, half, 0:HB, :]
            packed = kv[o, half, HB:HB + HR, :].astype(F32)
            parts = []
            for g in range(2):
                pg = packed[:, g * LANES:(g + 1) * LANES]
                for b in range(4):
                    parts.append(jnp.where(keep, pltpu.roll(pg, (NOPE - 32 * b) % LANES, 1), 0.0))
            rope = jnp.concatenate(parts, axis=0)
            k = dot(lat, ku[...])
            v = dot(lat, vu[...])
            rows = pl.ds(pl.multiple_of(o * R + half * HB, HB), HB)
            for h in range(H):
                kbuf[h, rows, :] = (k[:, h * LANES:(h + 1) * LANES] + rope).astype(BF)
                vbuf[h, rows, :] = (v[:, h * LANES:(h + 1) * LANES] + ones).astype(BF)

    scale = (NOPE + ROPE) ** -0.5

    def attend(row0, key0, count):
        qrows = pl.ds(row0, RG)
        krows = pl.ds(key0, count)
        for h in range(H):
            s = lax.dot_general(qbuf[h, qrows, :], kbuf[h, krows, :], (((1,), (1,)), ((), ())),
                                preferred_element_type=F32)
            old = mbuf[h]
            new = jnp.maximum(old, jnp.max(s, axis=1, keepdims=True))
            p = jnp.exp((s - new[:, 0:1]) * scale)
            shrink = jnp.exp((old - new) * scale)
            acc[h] = acc[h] * shrink + dot(p.astype(BF), vbuf[h, krows, :])
            mbuf[h] = new

    def reset():
        mbuf[...] = jnp.full(mbuf.shape, -jnp.inf, F32)
        acc[...] = jnp.zeros(acc.shape, F32)

    def finish(row0):
        rows = pl.ds(row0, RG)
        heads = []
        for h in range(H):
            a = acc[h]
            heads.append(a[:, :VDIM] / a[:, VDIM:VDIM + 1])
        attended = jnp.concatenate(heads, axis=1)
        mix[rows, C:] = gat[rows, :] * attended

    def row_of(k):
        return pl.multiple_of(k * RG, RG)

    def origin(s):
        step = jnp.where(s % 2 == 1, (s + 1) // 2, n_sp - s // 2)
        return (sp + step) % n_sp

    def block(k, which):
        rows = pl.ds(pl.multiple_of(k * RG + which * TB, TB), TB)
        return dot(mix[rows, :].astype(BF), w_down[...])

    def send_mate(d):
        return pltpu.make_async_remote_copy(
            src_ref=sbuf.at[d], dst_ref=pbuf.at[d], send_sem=dsend.at[d], recv_sem=drecv.at[d],
            device_id={"tp": mate}, device_id_type=MESH)

    def send_x(d):
        return pltpu.make_async_remote_copy(
            src_ref=xbuf.at[d], dst_ref=rbuf.at[d], send_sem=xsend.at[d], recv_sem=xrecv.at[d],
            device_id={"tp": ((chip + d) % X) * 2 + core}, device_id_type=MESH)

    def project_out(d):
        k = (chip + d) % X
        sbuf[d] = block(k, 1 - core).astype(BF)
        send_mate(d).start()
        ybuf[...] = block(k, core).astype(BF)

    def pair_sum(d):
        send_mate(d).wait_recv()
        return ybuf[...].astype(F32) + pbuf[d].astype(F32)

    first_chip = row_of((chip + 1) % X)
    reset()
    build(sp)
    attend(first_chip, pl.multiple_of(sp * R, R), R)

    o1 = origin(1)
    recv_kv(o1).wait_recv()
    relay_kv(o1, core).start()

    @pl.loop(1, n_sp)
    def _(s):
        o = origin(s)

        @pl.when(s + 1 < n_sp)
        def _():
            nxt = origin(s + 1)
            recv_kv(nxt).wait_recv()
            relay_kv(nxt, core).start()

        relay_kv(o, 1 - core).wait_recv()
        build(o)
        attend(first_chip, pl.multiple_of(o * R, R), R)

    finish(first_chip)

    send_halo(0).wait_recv()
    send_halo(1).wait_recv()
    cp = cprod[...].astype(F32)
    rid = lax.broadcasted_iota(jnp.int32, (R, C), 0)
    before = halo[0].astype(F32)[EDGE - 1:EDGE, :] * jnp.where(sp == 0, 0.0, 1.0)
    after = halo[1].astype(F32)[0:1, :] * jnp.where(sp == n_sp - 1, 0.0, 1.0)
    up = jnp.where(rid == 0, before, pltpu.roll(cp, 1, 0))
    down = jnp.where(rid == R - 1, after, pltpu.roll(cp, R - 1, 0))
    tw = taps[...].astype(F32)
    mix[:, 0:C] = cgo[...] * (up * tw[0:1] + cp * tw[1:2] + down * tw[2:3])

    loads[8].wait()
    loads[9].wait()
    CH = 2 if n_sp % 2 == 0 else 1
    for d in range(1, X + 1):
        e = d % X
        if X > 1:
            if d > 1:
                row0 = row_of((chip + e) % X)
                reset()

                @pl.loop(0, n_sp // CH)
                def _(s):
                    @pl.when(s == 1)
                    def _():
                        xbuf[d - 1] = pair_sum(d - 1).astype(BF)
                        send_x(d - 1).start()

                    attend(row0, pl.multiple_of(s * (CH * R), CH * R), CH * R)

                finish(row0)
        project_out(e)

    total = pair_sum(0)
    for d in range(1, X):
        send_x(d).wait_recv()
        total = total + rbuf[d].astype(F32)
    out[...] = total.astype(BF)

    for c in range(NC):
        send_tok(0, c).wait_send()
        for d in range(1, X):
            send_tok(d, c).wait_send()
            relay_tok(d, c).wait_send()
    for d in range(1, n_sp):
        send_kv(d).wait_send()
        relay_kv((sp + d) % n_sp, core).wait_send()
    send_halo(0).wait_send()
    send_halo(1).wait_send()
    for d in range(X):
        send_mate(d).wait_send()
    for d in range(1, X):
        send_x(d).wait_send()


def on_device(n_sp, n_tp, tokens, wci, wcn, wco, wcg, taps, wq, wl, wr, gain, ku, vu, wg, cd, ad):
    R, fl = tokens.shape
    D, C = wci.shape
    KV = wl.shape[1]
    H = ku.shape[1] // NOPE
    A = H * VDIM
    X = n_tp // 2
    RG, TB = R // X, R // n_tp
    NC = 4

    def by_head(w, width):
        w = w.reshape(w.shape[0], H, width)
        return jnp.pad(w, ((0, 0), (0, 0), (0, LANES - width))).reshape(w.shape[0], H * LANES)

    wq = by_head(wq, NOPE + ROPE)
    ku = by_head(ku, NOPE)
    vu = by_head(vu, VDIM)
    wr = jnp.pad(wr, ((0, 0), (NOPE, LANES - NOPE - ROPE)))
    HB = R // 2
    RB = HB + HB // 8
    S = n_sp * R
    dma = pltpu.SemaphoreType.DMA
    anys = pl.BlockSpec(memory_space=pl.ANY)
    vm = pl.BlockSpec(memory_space=pltpu.VMEM)
    V = pltpu.VMEM
    return pl.pallas_call(
        functools.partial(body, (n_sp, n_tp, R, fl, D, H, C, KV, NC)),
        out_shape=jax.ShapeDtypeStruct((TB, cd.shape[1]), BF),
        in_specs=[anys] * 11 + [vm] * 4,
        out_specs=vm,
        scratch_shapes=[
            V((R, D), BF), V((4, D, C), BF), V((D, H * LANES), BF), V((D, A), BF),
            V((D, KV + LANES), BF), V((C + A, cd.shape[1]), BF),
            V((n_sp, 2, RB, KV), BF), V((H, S, LANES), BF), V((H, S, LANES), BF),
            V((H, R, LANES), BF), V((R, LANES), F32), V((R, LANES), F32), V((R, LANES), F32),
            V((R, LANES), F32),
            V((R, C), BF), V((R, C), F32), V((R, A), F32), V((2, 16, C), BF), V((R, C + A), F32),
            V((H, RG, LANES), F32), V((H, RG, LANES), F32),
            V((X, TB, cd.shape[1]), BF), V((X, TB, cd.shape[1]), BF),
            V((X, TB, cd.shape[1]), BF), V((X, TB, cd.shape[1]), BF), V((TB, cd.shape[1]), BF),
            dma((11,)), dma((X, NC)), dma((X, NC)), dma((X, NC)), dma((X, NC)),
            dma((n_sp,)), dma((n_sp,)), dma((n_sp,)), dma((n_sp,)), dma((2,)), dma((2,)),
            dma((X,)), dma((X,)), dma((X,)), dma((X,)),
        ],
        compiler_params=pltpu.CompilerParams(
            collective_id=0, has_side_effects=True, vmem_limit_bytes=60 * 1024 * 1024),
    )(tokens, wci, wcn, wco, wcg, wq, wg, wl, wr, cd, ad, taps, gain.reshape(1, KV), ku, vu)


def solution(mesh):
    tp = P(None, "tp")
    placed = (P("sp", "tp"), tp, tp, tp, tp, tp, tp, P(), P(), P(), tp, tp, tp,
              P("tp", None), P("tp", None))
    return jax.shard_map(
        functools.partial(on_device, mesh.shape["sp"], mesh.shape["tp"]),
        mesh=mesh, in_specs=placed, out_specs=P(("sp", "tp"), None), check_vma=False)
```

```python
import functools
import math

import jax
import jax.numpy as jnp
from jax import lax
from jax.experimental import pallas as pl
from jax.experimental.pallas import tpu as pltpu
from jax.sharding import PartitionSpec as P

NOPE = 64
ROPE = 32
VDIM = 64
GRID_W = 64
LANES = 128
rms_eps = 1e-06
rope_theta = 10000.0
MESH = pl.DeviceIdType.MESH
BF = jnp.bfloat16
F32 = jnp.float32


def silu(v):
    return v / (1.0 + jnp.exp(-v))


def dot(a, b):
    return jnp.dot(a, b, preferred_element_type=F32)


def body(
    dims,
    tokens, wci, wcn, wco, wcg, wq, wg, wl, wr, cd, ad, ku, vu, taps, gain,
    out,
    x_all, w_conv, w_q, w_g, w_l, w_r, w_k, w_v, k_up, v_up, w_down, kv, kbuf, vbuf, qbuf, scl, cosb, sina, sinb,
    cprod, cgo, gat, halo, mix, mbuf, acc, sbuf, pbuf, xbuf, rbuf, ybuf,
    wsem, tsend, trecv, rsend, rrecv, ksend, krecv, psend, precv, hsend, hrecv,
    dsend, drecv, xsend, xrecv,
):
    n_sp, n_tp, R, fl, D, H, C, KV, NC = dims
    X = n_tp // 2
    RG = R // X
    TB = R // n_tp
    RC = R // NC
    HB = R // 2
    HR = HB // 8
    sp = lax.axis_index("sp")
    tp = lax.axis_index("tp")
    chip = tp // 2
    core = tp % 2
    mate = chip * 2 + (1 - core)

    loads = [
        pltpu.make_async_copy(wl, w_l, wsem.at[0]),
        pltpu.make_async_copy(wr, w_r, wsem.at[1]),
        pltpu.make_async_copy(wcn, w_conv.at[0], wsem.at[2]),
        pltpu.make_async_copy(wci, w_conv.at[1], wsem.at[3]),
        pltpu.make_async_copy(wco, w_conv.at[2], wsem.at[4]),
        pltpu.make_async_copy(wcg, w_conv.at[3], wsem.at[5]),
        pltpu.make_async_copy(wq, w_q, wsem.at[6]),
        pltpu.make_async_copy(wg, w_g, wsem.at[7]),
        pltpu.make_async_copy(cd, w_down.at[0:C, :], wsem.at[8]),
        pltpu.make_async_copy(ad, w_down.at[C:, :], wsem.at[9]),
        pltpu.make_async_copy(ku, w_k, wsem.at[11]),
        pltpu.make_async_copy(vu, w_v, wsem.at[12]),
    ]

    def cols(j):
        return pl.ds(pl.multiple_of(j * fl, fl), fl)

    own = pltpu.make_async_copy(tokens, x_all.at[:, cols(tp)], wsem.at[10])

    barrier = pltpu.get_barrier_semaphore()
    pl.semaphore_signal(barrier, inc=1, device_id={"tp": mate}, device_id_type=MESH)
    for d in range(1, X):
        peer = ((chip + d) % X) * 2 + core
        pl.semaphore_signal(barrier, inc=1, device_id={"tp": peer}, device_id_type=MESH)
    for d in range(1, n_sp):
        pl.semaphore_signal(barrier, inc=1, device_id={"sp": (sp + d) % n_sp}, device_id_type=MESH)
    own.start()
    pl.semaphore_wait(barrier, 1 + (X - 1) + (n_sp - 1))

    def send_tok(d, c):
        peer = mate if d == 0 else ((chip + d) % X) * 2 + core
        rows = pl.ds(c * RC, RC)
        return pltpu.make_async_remote_copy(
            src_ref=tokens.at[rows], dst_ref=x_all.at[rows, cols(tp)],
            send_sem=tsend.at[d, c], recv_sem=trecv.at[d, c],
            device_id={"tp": peer}, device_id_type=MESH)

    def relay_tok(d, c):
        origin = ((chip - d + X) % X) * 2 + core
        rows = pl.ds(c * RC, RC)
        part = x_all.at[rows, cols(origin)]
        return pltpu.make_async_remote_copy(
            src_ref=part, dst_ref=part,
            send_sem=rsend.at[d, c], recv_sem=rrecv.at[d, c],
            device_id={"tp": mate}, device_id_type=MESH)

    for c in range(NC):
        for d in range(1, X):
            send_tok(d, c).start()
    for c in range(NC):
        send_tok(0, c).start()
    for w in loads:
        w.start()

    lane = lax.broadcasted_iota(jnp.int32, (R, LANES), 1)
    pos = sp * R + lax.broadcasted_iota(jnp.int32, (R, LANES), 0)
    rl = lane - NOPE
    grid = jnp.where(rl < ROPE // 2, pos // GRID_W, pos % GRID_W).astype(F32)
    freq = jnp.exp((lane % 8).astype(F32) * (-math.log(rope_theta) / 8.0))
    ang = grid * freq
    active = (lane >= NOPE) & (lane < NOPE + ROPE)
    first = (lane % 16) < 8
    sin = jnp.sin(ang)
    cosb[...] = jnp.where(active, jnp.cos(ang), 0.0)
    sina[...] = jnp.where(active & first, -sin, 0.0)
    sinb[...] = jnp.where(active & (~first), sin, 0.0)

    def turned(v, rows):
        return (pltpu.roll(v, LANES - 8, 1) * sina[rows, :]
                + pltpu.roll(v, 8, 1) * sinb[rows, :])

    own.wait()
    loads[0].wait()
    loads[1].wait()
    for c in range(NC):
        for d in range(1, X):
            send_tok(d, c).wait_recv()
            relay_tok(d, c).start()
        send_tok(0, c).wait_recv()
        for d in range(1, X):
            relay_tok(d, c).wait_recv()
        rows = pl.ds(c * RC, RC)
        xr = x_all[rows, :]
        xf = xr.astype(F32)
        sc = lax.rsqrt(jnp.sum(xf * xf, axis=1, keepdims=True) * (1.0 / D) + rms_eps)
        scl[rows, :] = jnp.broadcast_to(sc, (RC, LANES))
        lat = dot(xr, w_l[...]) * sc
        lat = lat * lax.rsqrt(jnp.mean(lat * lat, axis=1, keepdims=True) + rms_eps) * gain[...]
        half, off = (c * RC) // HB, (c * RC) % HB
        kv[sp, half, off:off + RC, :] = lat.astype(BF)
        rp = jnp.concatenate([jnp.zeros((RC, NOPE), F32), lax.dot_general(
            xr, w_r[...], (((1,), (1,)), ((), ())), preferred_element_type=F32) * sc,
                              jnp.zeros((RC, LANES - NOPE - ROPE), F32)], axis=1)
        mix[rows, 0:LANES] = rp * cosb[rows, :] + turned(rp, rows)
    for half in range(2):
        packed = []
        for g in range(2):
            total = jnp.zeros((HR, LANES), F32)
            for b in range(4):
                r0 = half * HB + (g * 4 + b) * HR
                total = total + pltpu.roll(mix[r0:r0 + HR, 0:LANES], (32 * b - NOPE) % LANES, 1)
            packed.append(total)
        kv[sp, half, HB:HB + HR, :] = jnp.concatenate(packed, axis=1).astype(BF)

    def send_kv(d):
        part = kv.at[sp, core]
        return pltpu.make_async_remote_copy(
            src_ref=part, dst_ref=part, send_sem=ksend.at[d], recv_sem=krecv.at[sp],
            device_id={"sp": (sp + d) % n_sp}, device_id_type=MESH)

    def recv_kv(o):
        part = kv.at[o, core]
        return pltpu.make_async_remote_copy(
            src_ref=part, dst_ref=part, send_sem=ksend.at[0], recv_sem=krecv.at[o],
            device_id={"tp": mate}, device_id_type=MESH)

    def relay_kv(o, which):
        part = kv.at[o, which]
        return pltpu.make_async_remote_copy(
            src_ref=part, dst_ref=part, send_sem=psend.at[o], recv_sem=precv.at[o],
            device_id={"tp": mate}, device_id_type=MESH)

    order = []
    for i in range(1, n_sp):
        order.append((i + 1) // 2 if i % 2 else n_sp - i // 2)
    for d in order:
        send_kv(d).start()

    for w in loads[2:6]:
        w.wait()
    PB = min(R, 256)

    @pl.loop(0, R // PB)
    def _(i):
        rows = pl.ds(pl.multiple_of(i * PB, PB), PB)
        xr = x_all[rows, :]
        sc = scl[rows, 0:1]
        inner = (dot(xr, w_conv[0]) * sc).astype(BF).astype(F32)
        value = (dot(xr, w_conv[1]) * sc).astype(BF).astype(F32)
        cprod[rows, :] = (inner * value).astype(BF)
        outer = (dot(xr, w_conv[2]) * sc).astype(BF).astype(F32)
        gate = (dot(xr, w_conv[3]) * sc).astype(BF).astype(F32)
        cgo[rows, :] = silu(gate) * outer

    EDGE = 16
    HW = NOPE + ROPE

    def send_halo(k):
        src = cprod.at[pl.ds(R - EDGE, EDGE)] if k == 0 else cprod.at[pl.ds(0, EDGE)]
        to = (sp + 1) % n_sp if k == 0 else (sp + n_sp - 1) % n_sp
        return pltpu.make_async_remote_copy(
            src_ref=src, dst_ref=halo.at[k], send_sem=hsend.at[k], recv_sem=hrecv.at[k],
            device_id={"sp": to}, device_id_type=MESH)

    send_halo(0).start()
    send_halo(1).start()
    def origin(s):
        step = jnp.where(s % 2 == 1, (s + 1) // 2, n_sp - s // 2)
        return (sp + step) % n_sp

    o1 = origin(1)
    recv_kv(o1).wait_recv()
    relay_kv(o1, core).start()

    loads[6].wait()
    loads[7].wait()

    @pl.loop(0, R // PB)
    def _(i):
        rows = pl.ds(pl.multiple_of(i * PB, PB), PB)
        xr = x_all[rows, :]
        sc = scl[rows, 0:1]
        q = dot(xr, w_q[...]) * sc
        ln = lax.broadcasted_iota(jnp.int32, (PB, LANES), 1)
        for h in range(H):
            v = jnp.concatenate([q[:, h * HW:(h + 1) * HW], jnp.zeros((PB, LANES - HW), F32)], axis=1)
            v = v * jnp.where(ln < NOPE, 1.0, cosb[rows, :]) + turned(v, rows)
            qbuf[h, rows, :] = v.astype(BF)
        gat[rows, :] = silu((dot(xr, w_g[...]) * sc).astype(BF).astype(F32))

    loads[10].wait()
    loads[11].wait()
    for h in range(H):
        for raw, wide, width in ((w_k, k_up, NOPE), (w_v, v_up, VDIM)):
            piece = raw[:, h * width:(h + 1) * width].astype(F32)
            pad = jnp.zeros((KV, LANES - width), F32)
            wide[:, h * LANES:(h + 1) * LANES] = jnp.concatenate([piece, pad], axis=1).astype(BF)

    def build(o):
        ln = lax.broadcasted_iota(jnp.int32, (HR, LANES), 1)
        keep = (ln >= NOPE) & (ln < NOPE + ROPE)
        ones = jnp.where(lax.broadcasted_iota(jnp.int32, (HB, LANES), 1) == VDIM, 1.0, 0.0)
        for half in range(2):
            lat = kv[o, half, 0:HB, :]
            packed = kv[o, half, HB:HB + HR, :].astype(F32)
            parts = []
            for g in range(2):
                pg = packed[:, g * LANES:(g + 1) * LANES]
                for b in range(4):
                    parts.append(jnp.where(keep, pltpu.roll(pg, (NOPE - 32 * b) % LANES, 1), 0.0))
            rope = jnp.concatenate(parts, axis=0)
            k = dot(lat, k_up[...])
            v = dot(lat, v_up[...])
            rows = pl.ds(pl.multiple_of(o * R + half * HB, HB), HB)
            for h in range(H):
                kbuf[h, rows, :] = (k[:, h * LANES:(h + 1) * LANES] + rope).astype(BF)
                vbuf[h, rows, :] = (v[:, h * LANES:(h + 1) * LANES] + ones).astype(BF)

    scale = (NOPE + ROPE) ** -0.5 * math.log2(math.e)

    def attend(row0, key0, count):
        qrows = pl.ds(row0, RG)
        krows = pl.ds(key0, count)
        for h in range(H):
            s = lax.dot_general(qbuf[h, qrows, :], kbuf[h, krows, :], (((1,), (1,)), ((), ())),
                                preferred_element_type=F32)
            old = mbuf[h]
            new = jnp.maximum(old, jnp.max(s, axis=1, keepdims=True))
            p = jnp.exp2((s - new[:, 0:1]) * scale)
            shrink = jnp.exp2((old - new) * scale)
            acc[h] = acc[h] * shrink + dot(p.astype(BF), vbuf[h, krows, :])
            mbuf[h] = new

    def reset():
        mbuf[...] = jnp.full(mbuf.shape, -jnp.inf, F32)
        acc[...] = jnp.zeros(acc.shape, F32)

    def finish(row0):
        rows = pl.ds(row0, RG)
        heads = []
        for h in range(H):
            a = acc[h]
            heads.append(a[:, :VDIM] / a[:, VDIM:VDIM + 1])
        attended = jnp.concatenate(heads, axis=1)
        mix[rows, C:] = gat[rows, :] * attended

    def row_of(k):
        return pl.multiple_of(k * RG, RG)

    def block(k, which):
        rows = pl.ds(pl.multiple_of(k * RG + which * TB, TB), TB)
        return dot(mix[rows, :].astype(BF), w_down[...])

    def send_mate(d):
        return pltpu.make_async_remote_copy(
            src_ref=sbuf.at[d], dst_ref=pbuf.at[d], send_sem=dsend.at[d], recv_sem=drecv.at[d],
            device_id={"tp": mate}, device_id_type=MESH)

    def send_x(d):
        return pltpu.make_async_remote_copy(
            src_ref=xbuf.at[d], dst_ref=rbuf.at[d], send_sem=xsend.at[d], recv_sem=xrecv.at[d],
            device_id={"tp": ((chip + d) % X) * 2 + core}, device_id_type=MESH)

    def project_out(d):
        k = (chip + d) % X
        sbuf[d] = block(k, 1 - core).astype(BF)
        send_mate(d).start()
        ybuf[...] = block(k, core).astype(BF)

    def pair_sum(d):
        send_mate(d).wait_recv()
        return ybuf[...].astype(F32) + pbuf[d].astype(F32)

    first_chip = row_of((chip + 1) % X)
    reset()
    build(sp)
    attend(first_chip, pl.multiple_of(sp * R, R), R)

    @pl.loop(1, n_sp)
    def _(s):
        o = origin(s)

        @pl.when(s + 1 < n_sp)
        def _():
            nxt = origin(s + 1)
            recv_kv(nxt).wait_recv()
            relay_kv(nxt, core).start()

        relay_kv(o, 1 - core).wait_recv()
        build(o)
        attend(first_chip, pl.multiple_of(o * R, R), R)

    finish(first_chip)

    send_halo(0).wait_recv()
    send_halo(1).wait_recv()
    cp = cprod[...].astype(F32)
    rid = lax.broadcasted_iota(jnp.int32, (R, C), 0)
    before = halo[0].astype(F32)[EDGE - 1:EDGE, :] * jnp.where(sp == 0, 0.0, 1.0)
    after = halo[1].astype(F32)[0:1, :] * jnp.where(sp == n_sp - 1, 0.0, 1.0)
    up = jnp.where(rid == 0, before, pltpu.roll(cp, 1, 0))
    down = jnp.where(rid == R - 1, after, pltpu.roll(cp, R - 1, 0))
    tw = taps[...].astype(F32)
    mix[:, 0:C] = cgo[...] * (up * tw[0:1] + cp * tw[1:2] + down * tw[2:3])

    loads[8].wait()
    loads[9].wait()
    CH = 2 if n_sp % 2 == 0 else 1
    for d in range(1, X + 1):
        e = d % X
        if X > 1:
            if d > 1:
                row0 = row_of((chip + e) % X)
                reset()

                @pl.loop(0, n_sp // CH)
                def _(s):
                    @pl.when(s == 1)
                    def _():
                        xbuf[d - 1] = pair_sum(d - 1).astype(BF)
                        send_x(d - 1).start()

                    attend(row0, pl.multiple_of(s * (CH * R), CH * R), CH * R)

                finish(row0)
        project_out(e)

    total = pair_sum(0)
    for d in range(1, X):
        send_x(d).wait_recv()
        total = total + rbuf[d].astype(F32)
    out[...] = total.astype(BF)

    for c in range(NC):
        send_tok(0, c).wait_send()
        for d in range(1, X):
            send_tok(d, c).wait_send()
            relay_tok(d, c).wait_send()
    for d in range(1, n_sp):
        send_kv(d).wait_send()
        relay_kv((sp + d) % n_sp, core).wait_send()
    send_halo(0).wait_send()
    send_halo(1).wait_send()
    for d in range(X):
        send_mate(d).wait_send()
    for d in range(1, X):
        send_x(d).wait_send()


def on_device(n_sp, n_tp, tokens, wci, wcn, wco, wcg, taps, wq, wl, wr, gain, ku, vu, wg, cd, ad):
    R, fl = tokens.shape
    D, C = wci.shape
    KV = wl.shape[1]
    H = ku.shape[1] // NOPE
    A = H * VDIM
    X = n_tp // 2
    RG, TB = R // X, R // n_tp
    NC = 4

    HB = R // 2
    RB = HB + HB // 8
    S = n_sp * R
    dma = pltpu.SemaphoreType.DMA
    anys = pl.BlockSpec(memory_space=pl.ANY)
    vm = pl.BlockSpec(memory_space=pltpu.VMEM)
    V = pltpu.VMEM
    return pl.pallas_call(
        functools.partial(body, (n_sp, n_tp, R, fl, D, H, C, KV, NC)),
        out_shape=jax.ShapeDtypeStruct((TB, cd.shape[1]), BF),
        in_specs=[anys] * 13 + [vm] * 2,
        out_specs=vm,
        scratch_shapes=[
            V((R, D), BF), V((4, D, C), BF), V(wq.shape, BF), V((D, A), BF),
            V((D, KV), BF), V((ROPE, D), BF), V(ku.shape, BF), V(vu.shape, BF),
            V((KV, H * LANES), BF), V((KV, H * LANES), BF), V((C + A, cd.shape[1]), BF),
            V((n_sp, 2, RB, KV), BF), V((H, S, LANES), BF), V((H, S, LANES), BF),
            V((H, R, LANES), BF), V((R, LANES), F32), V((R, LANES), F32), V((R, LANES), F32),
            V((R, LANES), F32),
            V((R, C), BF), V((R, C), F32), V((R, A), F32), V((2, 16, C), BF), V((R, C + A), F32),
            V((H, RG, LANES), F32), V((H, RG, LANES), F32),
            V((X, TB, cd.shape[1]), BF), V((X, TB, cd.shape[1]), BF),
            V((X, TB, cd.shape[1]), BF), V((X, TB, cd.shape[1]), BF), V((TB, cd.shape[1]), BF),
            dma((13,)), dma((X, NC)), dma((X, NC)), dma((X, NC)), dma((X, NC)),
            dma((n_sp,)), dma((n_sp,)), dma((n_sp,)), dma((n_sp,)), dma((2,)), dma((2,)),
            dma((X,)), dma((X,)), dma((X,)), dma((X,)),
        ],
        compiler_params=pltpu.CompilerParams(
            collective_id=0, has_side_effects=True, vmem_limit_bytes=60 * 1024 * 1024),
    )(tokens, wci, wcn, wco, wcg, wq, wg, wl, wr.T, cd, ad, ku, vu, taps, gain.reshape(1, KV))


def solution(mesh):
    tp = P(None, "tp")
    placed = (P("sp", "tp"), tp, tp, tp, tp, tp, tp, P(), P(), P(), tp, tp, tp,
              P("tp", None), P("tp", None))
    return jax.shard_map(
        functools.partial(on_device, mesh.shape["sp"], mesh.shape["tp"]),
        mesh=mesh, in_specs=placed, out_specs=P(("sp", "tp"), None), check_vma=False)
```
